32 devices in a mesh: grp: 2 (over y), sp: 4 (over z), tp: 4 (over x, core).
Axes of the slice: x: 2, y: 2, z: 4, core: 2. Of those that a mesh axis runs over, the one named last changes fastest.
Arguments:
- tokens: bfloat16 [1024, 2048], P(('grp', 'sp'), 'tp'), parts along dimension 0, may hold values from -30 to 30, as said below
- norm_gain: float32 [2, 2048], replicated, may hold values from 0.1 to 1.9
- in_weight: bfloat16 [2, 2048, 2048], P(None, 'sp', 'tp'), may hold values from -0.125 to 0.125
- gate_weight: bfloat16 [2, 2048, 2048], P(None, 'sp', 'tp'), may hold values from -0.125 to 0.125
- conv_taps: float32 [2, 4, 2048], P(None, None, 'tp'), may hold values from -3 to 3
- decay_logit: float32 [2, 2, 2048], P(None, None, 'tp'), may hold values from 4 to 20, as said below
- gate_maps: bfloat16 [2, 2048, 1024], P(None, 'tp', 'sp'), may hold values from -0.375 to 0.375
- out_weight: bfloat16 [2, 2048, 2048], P(None, 'sp', 'tp'), may hold values from -0.375 to 0.375
- final_gain: float32 [2048], P('tp'), may hold values from 0.1 to 1.9
Outputs:
- normed_out: bfloat16 [1024, 2048], P(('grp', 'sp'), 'tp'), parts along dimension 0
The draws below stay inside these ranges and needn't reach their ends.
There are 2 independent parts, one for each index of `grp`. The reference program is written for one: setup_inputs(seed, part) draws one part's arguments, and reference() takes and returns one part's arrays. A program takes and returns all parts, laid end to end along the dimension named above; an argument that names none is the same for every part. Nothing has to cross between parts.
Inputs may be any that keep to these rules, and one draw needn't show every extreme that they name: Activations of order one whose scale changes by blocks of tokens and of channels. `decay_logit`: decay parameters; channels differ in how far their state reaches.
All inputs are finite; a program needn't handle non-finite values.
Results may differ from the reference program's by a relative error of at most 0.02.
Values may be sent and summed in bfloat16 or wider, within the bound.
No kernel may reach another device: no remote copies, remote signals or barrier semaphores. Data moves between devices by JAX's collectives and lax.ppermute only.
A program may use at most 128 MiB of HBM per device.

```python
import jax
import jax.numpy as jnp
from jax import lax

D = 2048
HEADS = 8
HEAD_W = 256
TAPS = 4
LAYERS = 2
TOK_DEV = 128
WIDTH_R = 2048
TOKENS = 512


def draw_tokens(key, part):
    first, second, third = jax.random.split(key, 3)
    base = jnp.clip(jax.random.normal(first, (TOKENS, D), jnp.float32), -5.0, 5.0)
    span = TOK_DEV // 2
    row_scale = jnp.exp(jax.random.uniform(second, (TOKENS // span,), jnp.float32, jnp.log(0.4), jnp.log(2.0)))
    col_scale = jnp.exp(jax.random.uniform(third, (8,), jnp.float32, jnp.log(0.35), jnp.log(2.8)))
    rows = jnp.repeat(row_scale, span)
    cols = jnp.repeat(col_scale, D // 8)
    return (base * rows[:, None] * cols[None, :]).astype(jnp.bfloat16)


def draw_decay_logit(key, part):
    first, second, third = jax.random.split(key, 3)
    shape = (LAYERS, 2, WIDTH_R)
    share = 0.5
    quick = jax.random.uniform(first, shape, jnp.float32) < share
    slow_rate = jnp.exp(jax.random.uniform(second, shape, jnp.float32, jnp.log(0.02), jnp.log(0.25))) / TOKENS
    quick_rate = jnp.exp(jax.random.uniform(third, shape, jnp.float32, jnp.log(0.0025), jnp.log(0.0083)))
    rate = jnp.where(quick, quick_rate, slow_rate)
    return -jnp.log(jnp.expm1(rate))


def levels(key, extent, pieces, low, high):
    gain, own = 1.0, jax.random.fold_in(key, 6)
    for axis_at, shards_of in pieces:
        heights = jnp.exp(jax.random.uniform(jax.random.fold_in(own, axis_at), (shards_of,), jnp.float32, low / len(pieces), high / len(pieces)))
        gain = gain * jnp.repeat(heights, extent[axis_at] // shards_of).reshape([-1 if axis == axis_at else 1 for axis in range(len(extent))])
    return gain


def bell_draw(rng, shape, spread, most, shards=(), dtype=jnp.bfloat16):
    level = levels(rng, shape, shards, -0.22, 0.18) if shards else 1.0
    values = jax.random.normal(rng, shape, jnp.float32) * spread * level
    return jnp.minimum(jnp.maximum(values, -most), most).astype(dtype)


def setup_inputs(seed: int = 0, part: int = 0) -> dict:
    key_of = jax.random.split(jax.random.key(seed), 10)
    own_keys = jax.random.split(jax.random.fold_in(key_of[9], part), 10)
    return {
        "tokens": draw_tokens(jax.random.fold_in(jax.random.fold_in(key_of[9], part), 71), part),
        "norm_gain": jnp.clip(1.0 + 0.18 * jax.random.normal(key_of[1], (LAYERS, D), jnp.float32), 0.1, 1.9),
        "in_weight": bell_draw(key_of[2], (LAYERS, D, WIDTH_R), D ** -0.5, 0.125, ((1, 4), (2, 4))),
        "gate_weight": bell_draw(key_of[3], (LAYERS, D, WIDTH_R), D ** -0.5, 0.125, ((1, 4), (2, 4))),
        "conv_taps": bell_draw(key_of[4], (LAYERS, TAPS, WIDTH_R), 0.5, 3.0, ((2, 4),), jnp.float32),
        "decay_logit": draw_decay_logit(jax.random.fold_in(key_of[9], 71), part),
        "gate_maps": bell_draw(key_of[6], (LAYERS, WIDTH_R, 4 * HEAD_W), HEAD_W ** -0.5, 0.375, ((1, 4), (2, 4))),
        "out_weight": bell_draw(key_of[7], (LAYERS, WIDTH_R, D), (WIDTH_R // 8) ** -0.5, 0.375, ((1, 4), (2, 4))),
        "final_gain": jnp.clip(1.0 + 0.18 * jax.random.normal(key_of[8], (D,), jnp.float32), 0.1, 1.9),
    }


EPS = 1e-06

def combine_pair(earlier, later):
    return (earlier[0] * later[0], later[0] * earlier[1] + later[1])

def reference(tokens, norm_gain, in_weight, gate_weight, conv_taps, decay_logit, gate_maps, out_weight, final_gain):
    resid = tokens
    length = tokens.shape[0]
    for layer in range(LAYERS):
        wide = resid.astype(jnp.float32)
        normed = (wide * lax.rsqrt(lax.optimization_barrier(jnp.mean(wide * wide, axis=1, keepdims=True)) + EPS) * norm_gain[layer]).astype(jnp.bfloat16)
        xin = jnp.dot(normed, in_weight[layer], preferred_element_type=jnp.float32).astype(jnp.bfloat16)
        gin = jnp.dot(normed, gate_weight[layer], preferred_element_type=jnp.float32).astype(jnp.bfloat16)
        padded = jnp.pad(xin.astype(jnp.float32), ((2, 1), (0, 0)))
        conv = conv_taps[layer, 0] * padded[0:length]
        for k in range(1, TAPS):
            conv = conv + conv_taps[layer, k] * padded[k:k + length]
        conv = conv.astype(jnp.bfloat16)
        stacked = conv.astype(jnp.float32).reshape(length, HEADS, HEAD_W)
        maps = gate_maps[layer].astype(jnp.float32).reshape(HEADS, HEAD_W, 4 * HEAD_W)
        pre = jnp.einsum('thi,hij->thj', stacked, maps).reshape(length, HEADS, 4, HEAD_W)
        conv32 = conv.astype(jnp.float32)
        states = []
        for direction in range(2):
            rate = jax.nn.sigmoid(pre[:, :, 2 * direction]).reshape(length, WIDTH_R)
            inp = jax.nn.sigmoid(pre[:, :, 2 * direction + 1]).reshape(length, WIDTH_R)
            log_a = -8.0 * rate * jax.nn.softplus(-decay_logit[layer, direction])
            decay = jnp.exp(log_a)
            drive = jnp.sqrt(-jnp.expm1(2.0 * log_a)) * inp * conv32
            _, state = lax.associative_scan(combine_pair, (decay, drive), reverse=direction == 1, axis=0)
            states.append(state)
        mix = (jax.nn.gelu(gin.astype(jnp.float32)) * (states[0] + states[1])).astype(jnp.bfloat16)
        out = jnp.dot(mix, out_weight[layer], preferred_element_type=jnp.float32)
        resid = (resid.astype(jnp.float32) + out).astype(jnp.bfloat16)
    wide = resid.astype(jnp.float32)
    return (wide * lax.rsqrt(lax.optimization_barrier(jnp.mean(wide * wide, axis=1, keepdims=True)) + EPS) * final_gain).astype(jnp.bfloat16)
```

```python
import jax
import jax.numpy as jnp
from jax import lax
from jax.experimental import pallas as pl
from jax.experimental.pallas import tpu as pltpu
from jax.sharding import PartitionSpec as P

D = 2048
HEAD_W = 256
TAPS = 4
LAYERS = 2
SEGS = 8

EPS = 1e-06
BF = jnp.bfloat16
F32 = jnp.float32


def conv_kernel(*refs):
    pieces = refs[:-4]
    scale_ref, taps_ref, conv_ref, gin_ref = refs[-4:]
    total = pieces[0][...].astype(F32)
    for piece in pieces[1:]:
        total = total + piece[...].astype(F32)
    total = total * scale_ref[...]
    length, width = conv_ref.shape
    gin_ref[...] = total[:, width:].astype(BF)
    xin = total[:, :width].astype(BF).astype(F32)
    row = lax.broadcasted_iota(jnp.int32, (length, width), 0)
    conv = None
    for k in range(TAPS):
        off = k - 2
        shifted = xin if off == 0 else pltpu.roll(xin, (-off) % length, 0)
        if off < 0:
            shifted = jnp.where(row >= -off, shifted, 0.0)
        elif off > 0:
            shifted = jnp.where(row < length - off, shifted, 0.0)
        term = taps_ref[k : k + 1, :] * shifted
        conv = term if conv is None else conv + term
    conv_ref[...] = conv.astype(BF)


def neg_expm1(y):
    series = 1.0 + y * (1.0 / 8.0)
    for n in range(7, 1, -1):
        series = 1.0 + y * (1.0 / n) * series
    return jnp.where(y > -0.5, -y * series, 1.0 - jnp.exp(y))


def scan_kernel(head_ref, conv_ref, gin_ref, maps_ref, coef_ref, mix_ref, a0, b0, a1, b1):
    length, width = conv_ref.shape
    steps = length // SEGS
    conv = conv_ref[...].astype(F32)
    pre = jnp.dot(head_ref[...], maps_ref[...], preferred_element_type=F32)
    for d, (a_ref, b_ref) in enumerate(((a0, b0), (a1, b1))):
        rate = jax.nn.sigmoid(pre[:, (2 * d) * width : (2 * d + 1) * width])
        inp = jax.nn.sigmoid(pre[:, (2 * d + 1) * width : (2 * d + 2) * width])
        log_a = rate * coef_ref[d : d + 1, :]
        a_ref[...] = jnp.exp(log_a)
        b_ref[...] = jnp.sqrt(neg_expm1(2.0 * log_a)) * inp * conv

    def step(j, state):
        pf, hf, pb, hb = state
        at = pl.ds(j, SEGS, stride=steps)
        back = pl.ds(steps - 1 - j, SEGS, stride=steps)
        af = a0[at, :]
        ab = a1[back, :]
        hf = af * hf + b0[at, :]
        hb = ab * hb + b1[back, :]
        pf = af * pf
        pb = ab * pb
        a0[at, :] = pf
        b0[at, :] = hf
        a1[back, :] = pb
        b1[back, :] = hb
        return pf, hf, pb, hb

    one = jnp.ones((SEGS, width), F32)
    zero = jnp.zeros((SEGS, width), F32)
    pf, hf, pb, hb = lax.fori_loop(0, steps, step, (one, zero, one, zero), unroll=8)
    carry = jnp.zeros((1, width), F32)
    fwd = []
    for s in range(SEGS):
        fwd.append(carry)
        carry = pf[s : s + 1] * carry + hf[s : s + 1]
    carry = jnp.zeros((1, width), F32)
    bwd = [None] * SEGS
    for s in reversed(range(SEGS)):
        bwd[s] = carry
        carry = pb[s : s + 1] * carry + hb[s : s + 1]
    for s in range(SEGS):
        rows = slice(s * steps, (s + 1) * steps)
        hidden = b0[rows, :] + a0[rows, :] * fwd[s] + b1[rows, :] + a1[rows, :] * bwd[s]
        gate = jax.nn.gelu(gin_ref[rows, :].astype(F32), approximate=True)
        mix_ref[rows, :] = (gate * hidden).astype(BF)


def conv_call(pieces, scale, taps):
    length, width = pieces[0].shape[0], taps.shape[1]
    out = jax.ShapeDtypeStruct((length, width), BF)
    return pl.pallas_call(conv_kernel, out_shape=(out, out), name="conv")(*pieces, scale, taps)


def scan_call(head, conv, gin, maps, coef):
    return pl.pallas_call(
        scan_kernel,
        out_shape=jax.ShapeDtypeStruct(conv.shape, BF),
        scratch_shapes=[pltpu.VMEM(conv.shape, F32)] * 4,
        name="scan",
    )(head, conv, gin, maps, coef)


def body_square(
    tokens,
    norm_gain,
    in_weight,
    gate_weight,
    conv_taps,
    decay_logit,
    gate_maps,
    out_weight,
    final_gain,
):
    n = lax.axis_size("sp")
    s = lax.axis_index("sp")
    q = lax.axis_index("tp")
    rows, block = tokens.shape
    width = block // n
    group = HEAD_W // width
    axes = ("sp", "tp")
    swap = [(a * n + b, b * n + a) for a in range(n) for b in range(n)]
    to_piece = [[(a * n + b, b * n + (a - k) % n) for a in range(n) for b in range(n)] for k in range(n)]
    rotate = [[(a, (a + k) % n) for a in range(n)] for k in range(n)]
    sets = [[g * group + i for i in range(group)] for g in range(n // group)]

    def scatter(make):
        return [lax.ppermute(make((s - k) % n), axes, to_piece[k]) for k in range(n)]

    def cols(value, at, size):
        return lax.dynamic_slice_in_dim(value, at * size, size, value.ndim - 1)

    turned = lax.ppermute(tokens, axes, swap)
    small = jnp.concatenate([conv_taps, decay_logit], axis=1)
    small = cols(lax.ppermute(small, axes, swap), q, width)
    full = lax.all_gather(turned, "tp", axis=0, tiled=True)
    own = cols(full, q, width)
    gain = cols(norm_gain, s, block)

    def maps_of(layer):
        held = gate_maps[layer]

        def cut(piece):
            at = (piece // group * HEAD_W, piece % group * width)
            return lax.dynamic_slice(held, at, (HEAD_W, width))

        got = scatter(cut)
        ordered = jnp.stack(got)
        ordered = jnp.stack([lax.dynamic_index_in_dim(ordered, (g - q) % n, 0, False) for g in range(n)], 1)
        return ordered.reshape(HEAD_W, n * width)

    for layer in range(LAYERS):
        wide = full.astype(F32)
        part = jnp.sum(wide * wide, axis=1)
        total = part
        for k in range(1, n):
            total = total + lax.ppermute(part, "sp", rotate[k])
        scale = lax.rsqrt(total / D + EPS)[:, None]
        scaled = (wide * gain[layer]).astype(BF)

        def project(piece):
            w = jnp.concatenate(
                [cols(in_weight[layer], piece, width), cols(gate_weight[layer], piece, width)], axis=1
            )
            return jnp.dot(scaled, w, preferred_element_type=F32).astype(BF)

        conv, gin = conv_call(scatter(project), scale, small[layer, :TAPS])
        head = conv
        if group > 1:
            head = lax.all_gather(conv, "tp", axis=1, tiled=True, axis_index_groups=sets)
        coef = -8.0 * jax.nn.softplus(-small[layer, TAPS:])
        mix = scan_call(head, conv, gin, maps_of(layer), coef)
        mixed = lax.all_gather(mix, "tp", axis=1, tiled=True)
        if layer + 1 < LAYERS:
            pieces = scatter(
                lambda piece: jnp.dot(
                    mixed, cols(out_weight[layer], piece, width), preferred_element_type=F32
                ).astype(BF)
            )
            out = own.astype(F32)
            for piece in pieces:
                out = out + piece.astype(F32)
            own = out.astype(BF)
            full = lax.all_gather(own, "tp", axis=1, tiled=True)
        else:
            here = (s == q).astype(F32)

            def part_for(dest):
                m = lax.dynamic_slice_in_dim(mixed, dest * rows, rows, 0)
                r = lax.dynamic_slice_in_dim(full, dest * rows, rows, 0)
                return jnp.dot(m, out_weight[layer], preferred_element_type=F32) + here * r.astype(F32)

            sent = [lax.ppermute(part_for((s + k) % n).astype(BF), "sp", rotate[k]) for k in range(1, n)]
            out = part_for(s)
            for piece in sent:
                out = out + piece.astype(F32)
            resid = out.astype(BF)
    wide = resid.astype(F32)
    part = jnp.sum(wide * wide, axis=1)
    total = part
    for k in range(1, n):
        total = total + lax.ppermute(part, "tp", rotate[k])
    scale = lax.rsqrt(total / D + EPS)
    return (wide * scale[:, None] * final_gain).astype(BF)


def extended(value, sides, width):
    for axis, dim in sides:
        devices, length = (lax.axis_size(axis), value.shape[dim])
        up = [(i, (i + 1) % devices) for i in range(devices - 1)]
        down = [(j, i) for i, j in up]
        last = lax.slice_in_dim(value, length - width, length, axis=dim)
        leading = lax.slice_in_dim(value, 0, width, axis=dim)
        before = lax.ppermute(last, axis, up)
        after = lax.ppermute(leading, axis, down)
        value = jnp.concatenate([before, value, after], axis=dim)
    return value


def combine_pair(earlier, later):
    return (earlier[0] * later[0], later[0] * earlier[1] + later[1])


def body(
    tokens,
    norm_gain,
    in_weight,
    gate_weight,
    conv_taps,
    decay_logit,
    gate_maps,
    out_weight,
    final_gain,
):
    resid = tokens
    rows = tokens.shape[0]
    width = in_weight.shape[2]
    local_heads = width // HEAD_W
    for layer in range(LAYERS):
        whole = lax.all_gather(resid, "tp", axis=1, tiled=True)
        wide = whole.astype(jnp.float32)
        normed = (
            wide * lax.rsqrt(jnp.mean(wide * wide, axis=1, keepdims=True) + EPS) * norm_gain[layer]
        ).astype(jnp.bfloat16)
        proj_in = jnp.dot(
            normed,
            lax.all_gather(in_weight[layer], "sp", axis=0, tiled=True),
            preferred_element_type=jnp.float32,
        )
        proj_gate = jnp.dot(
            normed,
            lax.all_gather(gate_weight[layer], "sp", axis=0, tiled=True),
            preferred_element_type=jnp.float32,
        )
        xin = proj_in.astype(jnp.bfloat16)
        gin = proj_gate.astype(jnp.bfloat16)
        padded = extended(xin, (("sp", 0),), 2).astype(jnp.float32)
        conv = conv_taps[layer, 0] * padded[0:rows]
        for k in range(1, TAPS):
            conv = conv + conv_taps[layer, k] * padded[k : k + rows]
        conv = conv.astype(jnp.bfloat16)
        stacked = conv.reshape(rows, local_heads, HEAD_W)
        piece = lax.all_gather(gate_maps[layer], "sp", axis=1, tiled=True)
        blocks = piece.reshape(local_heads, HEAD_W, piece.shape[1])
        pre = jnp.einsum("thi,hij->thj", stacked, blocks, preferred_element_type=jnp.float32)
        pre = pre.reshape(rows, local_heads, 4, HEAD_W)
        conv32 = conv.astype(jnp.float32)
        locals_a = []
        locals_h = []
        for direction in range(2):
            rate = jax.nn.sigmoid(pre[:, :, 2 * direction]).reshape(rows, width)
            inp = jax.nn.sigmoid(pre[:, :, 2 * direction + 1]).reshape(rows, width)
            log_a = -8.0 * rate * jax.nn.softplus(-decay_logit[layer, direction])
            decay = jnp.exp(log_a)
            drive = jnp.sqrt(-jnp.expm1(2.0 * log_a)) * inp * conv32
            prod_a, state = lax.associative_scan(
                combine_pair, (decay, drive), reverse=direction == 1, axis=0
            )
            locals_a.append(prod_a)
            locals_h.append(state)
        summary = jnp.stack([locals_a[0][-1], locals_h[0][-1], locals_a[1][0], locals_h[1][0]])[
            None
        ]
        every = lax.all_gather(summary, "sp", axis=0, tiled=True)
        count = every.shape[0]
        me = lax.axis_index("sp")
        _, incl_f = lax.associative_scan(combine_pair, (every[:, 0], every[:, 1]), axis=0)
        _, incl_b = lax.associative_scan(
            combine_pair, (every[:, 2], every[:, 3]), reverse=True, axis=0
        )
        before = lax.dynamic_index_in_dim(incl_f, jnp.maximum(me - 1, 0), 0, keepdims=False)
        after = lax.dynamic_index_in_dim(incl_b, jnp.minimum(me + 1, count - 1), 0, keepdims=False)
        carry_f = before * (me > 0).astype(jnp.float32)
        carry_b = after * (me < count - 1).astype(jnp.float32)
        hidden = locals_h[0] + locals_a[0] * carry_f + locals_h[1] + locals_a[1] * carry_b
        mix = (jax.nn.gelu(gin.astype(jnp.float32)) * hidden).astype(jnp.bfloat16)
        full_mix = lax.all_gather(mix, "tp", axis=1, tiled=True)
        out = jnp.dot(
            full_mix,
            lax.all_gather(out_weight[layer], "sp", axis=0, tiled=True),
            preferred_element_type=jnp.float32,
        )
        resid = (resid.astype(jnp.float32) + out).astype(jnp.bfloat16)
    wide = resid.astype(jnp.float32)
    total = lax.psum(jnp.sum(wide * wide, axis=1), "tp")
    scale = lax.rsqrt(total / D + EPS)
    return (wide * scale[:, None] * final_gain).astype(jnp.bfloat16)


def solution(mesh):
    placed = (
        P(("grp", "sp"), "tp"),
        P(),
        P(None, "sp", "tp"),
        P(None, "sp", "tp"),
        P(None, None, "tp"),
        P(None, None, "tp"),
        P(None, "tp", "sp"),
        P(None, "sp", "tp"),
        P("tp"),
    )
    n = mesh.shape["sp"]
    square = n == mesh.shape["tp"] and n == 4 and HEAD_W % (D // (n * n)) == 0
    return jax.shard_map(
        body_square if square else body,
        mesh=mesh,
        in_specs=placed,
        out_specs=P(("grp", "sp"), "tp"),
        check_vma=False,
    )
```

```python
import jax
import jax.numpy as jnp
from jax import lax
from jax.experimental import pallas as pl
from jax.experimental.pallas import tpu as pltpu
from jax.sharding import PartitionSpec as P

D = 2048
HEAD_W = 256
TAPS = 4
LAYERS = 2
SEGS = 8

EPS = 1e-06
BF = jnp.bfloat16
F32 = jnp.float32


def conv_kernel(*refs):
    pieces = refs[:-3]
    scale_ref, taps_ref, conv_ref = refs[-3:]
    total = pieces[0][...].astype(F32)
    for piece in pieces[1:]:
        total = total + piece[...].astype(F32)
    length, width = conv_ref.shape
    xin = (total * scale_ref[...]).astype(BF).astype(F32)
    row = lax.broadcasted_iota(jnp.int32, (length, width), 0)
    conv = None
    for k in range(TAPS):
        off = k - 2
        shifted = xin if off == 0 else pltpu.roll(xin, (-off) % length, 0)
        if off < 0:
            shifted = jnp.where(row >= -off, shifted, 0.0)
        elif off > 0:
            shifted = jnp.where(row < length - off, shifted, 0.0)
        term = taps_ref[k : k + 1, :] * shifted
        conv = term if conv is None else conv + term
    conv_ref[...] = conv.astype(BF)


def neg_expm1(y):
    series = 1.0 + y * (1.0 / 8.0)
    for n in range(7, 1, -1):
        series = 1.0 + y * (1.0 / n) * series
    return jnp.where(y > -0.5, -y * series, 1.0 - jnp.exp(y))


def scan_kernel(head_ref, conv_ref, maps_ref, coef_ref, hidden_ref, a0, b0, a1, b1):
    length, width = conv_ref.shape
    steps = length // SEGS
    conv = conv_ref[...].astype(F32)
    pre = jnp.dot(head_ref[...], maps_ref[...], preferred_element_type=F32)
    for d, (a_ref, b_ref) in enumerate(((a0, b0), (a1, b1))):
        rate = jax.nn.sigmoid(pre[:, (2 * d) * width : (2 * d + 1) * width])
        inp = jax.nn.sigmoid(pre[:, (2 * d + 1) * width : (2 * d + 2) * width])
        log_a = rate * coef_ref[d : d + 1, :]
        a_ref[...] = jnp.exp(log_a)
        b_ref[...] = jnp.sqrt(neg_expm1(2.0 * log_a)) * inp * conv

    def step(j, state):
        pf, hf, pb, hb = state
        at = pl.ds(j, SEGS, stride=steps)
        back = pl.ds(steps - 1 - j, SEGS, stride=steps)
        af = a0[at, :]
        ab = a1[back, :]
        hf = af * hf + b0[at, :]
        hb = ab * hb + b1[back, :]
        pf = af * pf
        pb = ab * pb
        a0[at, :] = pf
        b0[at, :] = hf
        a1[back, :] = pb
        b1[back, :] = hb
        return pf, hf, pb, hb

    one = jnp.ones((SEGS, width), F32)
    zero = jnp.zeros((SEGS, width), F32)
    pf, hf, pb, hb = lax.fori_loop(0, steps, step, (one, zero, one, zero), unroll=8)
    carry = jnp.zeros((1, width), F32)
    fwd = []
    for s in range(SEGS):
        fwd.append(carry)
        carry = pf[s : s + 1] * carry + hf[s : s + 1]
    carry = jnp.zeros((1, width), F32)
    bwd = [None] * SEGS
    for s in reversed(range(SEGS)):
        bwd[s] = carry
        carry = pb[s : s + 1] * carry + hb[s : s + 1]
    for s in range(SEGS):
        rows = slice(s * steps, (s + 1) * steps)
        hidden_ref[rows, :] = (
            b0[rows, :] + a0[rows, :] * fwd[s] + b1[rows, :] + a1[rows, :] * bwd[s]
        )


def conv_call(pieces, scale, taps):
    length, width = pieces[0].shape[0], taps.shape[1]
    out = jax.ShapeDtypeStruct((length, width), BF)
    return pl.pallas_call(conv_kernel, out_shape=out, name="conv")(*pieces, scale, taps)


def scan_call(head, conv, maps, coef):
    return pl.pallas_call(
        scan_kernel,
        out_shape=jax.ShapeDtypeStruct(conv.shape, F32),
        scratch_shapes=[pltpu.VMEM(conv.shape, F32)] * 4,
        name="scan",
    )(head, conv, maps, coef)


def body_square(
    tokens,
    norm_gain,
    in_weight,
    gate_weight,
    conv_taps,
    decay_logit,
    gate_maps,
    out_weight,
    final_gain,
):
    n = lax.axis_size("sp")
    s = lax.axis_index("sp")
    q = lax.axis_index("tp")
    rows, block = tokens.shape
    width = block // n
    group = HEAD_W // width
    axes = ("sp", "tp")
    swap = [(a * n + b, b * n + a) for a in range(n) for b in range(n)]
    to_piece = [[(a * n + b, b * n + (a - k) % n) for a in range(n) for b in range(n)] for k in range(n)]
    rotate = [[(a, (a + k) % n) for a in range(n)] for k in range(n)]
    sets = [[g * group + i for i in range(group)] for g in range(n // group)]

    def scatter(make):
        return [lax.ppermute(make((s - k) % n), axes, to_piece[k]) for k in range(n)]

    half = n // 2
    flip = [(b, (b + half) % n) for b in range(n)]
    side = q // half
    by_side = [[] for _ in range(n)]
    for k in range(n):
        for a in range(n):
            for b in range(n):
                kind, core = ((a ^ k) % 2, (a ^ k) // 2)
                dest = (b + kind * half) % n
                by_side[k].append((a * n + b, dest * n + b // half * half + core))

    def scatter_sides(make):
        other = jnp.stack([make((1 - side) * half + c) for c in range(half)])
        passed = lax.ppermute(other, "tp", flip)
        held = jnp.stack([v for c in range(half) for v in (make(side * half + c), passed[c])])
        return [lax.dynamic_index_in_dim(held, s ^ k, 0, False) for k in range(n)]

    def gather_cols(value, sets=None):
        got = lax.all_gather(value, "tp", axis=0, axis_index_groups=sets)
        return jnp.concatenate([got[i] for i in range(got.shape[0])], axis=1)

    def cols(value, at, size):
        return lax.dynamic_slice_in_dim(value, at * size, size, value.ndim - 1)

    turned = lax.ppermute(tokens, axes, swap)
    gain = cols(norm_gain, s, block)

    def cuts_of(held):
        def cut(piece):
            at = (piece // group * HEAD_W, piece % group * width)
            return lax.dynamic_slice(held, at, (HEAD_W, width))

        return [cut((s - k) % n) for k in range(n)]

    def maps_of(cuts):
        got = [lax.ppermute(cuts[k], axes, to_piece[k]) for k in range(n)]
        ordered = jnp.stack(got)
        ordered = jnp.stack([lax.dynamic_index_in_dim(ordered, (g - q) % n, 0, False) for g in range(n)], 1)
        return ordered.reshape(HEAD_W, n * width)

    small = jnp.concatenate([conv_taps, decay_logit], axis=1)
    cuts = cuts_of(gate_maps[0])
    small, cuts, turned = lax.optimization_barrier((small, cuts, turned))
    maps = maps_of(cuts)
    small = cols(lax.ppermute(small, axes, swap), q, width)
    full = lax.all_gather(turned, "tp", axis=0, tiled=True)
    own = cols(full, q, width)

    for layer in range(LAYERS):
        wide = full.astype(F32)
        part = jnp.sum(wide * wide, axis=1)
        total = part
        for k in range(1, n):
            total = total + lax.ppermute(part, "sp", rotate[k])
        scale = lax.rsqrt(total / D + EPS)[:, None]
        scaled = (wide * gain[layer]).astype(BF)

        def project(weight, value):
            return lambda piece: jnp.dot(
                value, cols(weight, piece, width), preferred_element_type=F32
            ).astype(BF)

        xparts = [project(in_weight[layer], scaled)((s - k) % n) for k in range(n)]
        xparts, scaled = lax.optimization_barrier((xparts, scaled))
        conv = conv_call(
            [lax.ppermute(xparts[k], axes, to_piece[k]) for k in range(n)],
            scale,
            small[layer, :TAPS],
        )
        gins = scatter_sides(project(gate_weight[layer], scaled))
        gins, conv = lax.optimization_barrier((gins, conv))
        gins = [lax.ppermute(gins[k], axes, by_side[k]) for k in range(n)]
        head = gather_cols(conv, sets) if group > 1 else conv
        coef = -8.0 * jax.nn.softplus(-small[layer, TAPS:])
        hidden = scan_call(head, conv, maps, coef)
        gin = gins[0].astype(F32)
        for piece in gins[1:]:
            gin = gin + piece.astype(F32)
        gin = (gin * scale).astype(BF).astype(F32)
        mix = (jax.nn.gelu(gin, approximate=True) * hidden).astype(BF)
        if layer + 1 < LAYERS:
            cuts, mix = lax.optimization_barrier((cuts_of(gate_maps[layer + 1]), mix))
            maps = maps_of(cuts)
        mixed = gather_cols(mix)
        if layer + 1 < LAYERS:
            pieces = scatter(
                lambda piece: jnp.dot(
                    mixed, cols(out_weight[layer], piece, width), preferred_element_type=F32
                ).astype(BF)
            )
            out = own.astype(F32)
            for piece in pieces:
                out = out + piece.astype(F32)
            own = out.astype(BF)
            full = gather_cols(own)
        else:
            here = (s == q).astype(F32)

            def part_for(dest):
                m = lax.dynamic_slice_in_dim(mixed, dest * rows, rows, 0)
                r = lax.dynamic_slice_in_dim(full, dest * rows, rows, 0)
                return jnp.dot(m, out_weight[layer], preferred_element_type=F32) + here * r.astype(F32)

            sent = [lax.ppermute(part_for((s + k) % n).astype(BF), "sp", rotate[k]) for k in range(1, n)]
            out = part_for(s)
            for piece in sent:
                out = out + piece.astype(F32)
            resid = out.astype(BF)
    wide = resid.astype(F32)
    part = jnp.sum(wide * wide, axis=1)
    total = part
    for k in range(1, n):
        total = total + lax.ppermute(part, "tp", rotate[k])
    scale = lax.rsqrt(total / D + EPS)
    return (wide * scale[:, None] * final_gain).astype(BF)


def extended(value, sides, width):
    for axis, dim in sides:
        devices, length = (lax.axis_size(axis), value.shape[dim])
        up = [(i, (i + 1) % devices) for i in range(devices - 1)]
        down = [(j, i) for i, j in up]
        last = lax.slice_in_dim(value, length - width, length, axis=dim)
        leading = lax.slice_in_dim(value, 0, width, axis=dim)
        before = lax.ppermute(last, axis, up)
        after = lax.ppermute(leading, axis, down)
        value = jnp.concatenate([before, value, after], axis=dim)
    return value


def combine_pair(earlier, later):
    return (earlier[0] * later[0], later[0] * earlier[1] + later[1])


def body(
    tokens,
    norm_gain,
    in_weight,
    gate_weight,
    conv_taps,
    decay_logit,
    gate_maps,
    out_weight,
    final_gain,
):
    resid = tokens
    rows = tokens.shape[0]
    width = in_weight.shape[2]
    local_heads = width // HEAD_W
    for layer in range(LAYERS):
        whole = lax.all_gather(resid, "tp", axis=1, tiled=True)
        wide = whole.astype(jnp.float32)
        normed = (
            wide * lax.rsqrt(jnp.mean(wide * wide, axis=1, keepdims=True) + EPS) * norm_gain[layer]
        ).astype(jnp.bfloat16)
        proj_in = jnp.dot(
            normed,
            lax.all_gather(in_weight[layer], "sp", axis=0, tiled=True),
            preferred_element_type=jnp.float32,
        )
        proj_gate = jnp.dot(
            normed,
            lax.all_gather(gate_weight[layer], "sp", axis=0, tiled=True),
            preferred_element_type=jnp.float32,
        )
        xin = proj_in.astype(jnp.bfloat16)
        gin = proj_gate.astype(jnp.bfloat16)
        padded = extended(xin, (("sp", 0),), 2).astype(jnp.float32)
        conv = conv_taps[layer, 0] * padded[0:rows]
        for k in range(1, TAPS):
            conv = conv + conv_taps[layer, k] * padded[k : k + rows]
        conv = conv.astype(jnp.bfloat16)
        stacked = conv.reshape(rows, local_heads, HEAD_W)
        piece = lax.all_gather(gate_maps[layer], "sp", axis=1, tiled=True)
        blocks = piece.reshape(local_heads, HEAD_W, piece.shape[1])
        pre = jnp.einsum("thi,hij->thj", stacked, blocks, preferred_element_type=jnp.float32)
        pre = pre.reshape(rows, local_heads, 4, HEAD_W)
        conv32 = conv.astype(jnp.float32)
        locals_a = []
        locals_h = []
        for direction in range(2):
            rate = jax.nn.sigmoid(pre[:, :, 2 * direction]).reshape(rows, width)
            inp = jax.nn.sigmoid(pre[:, :, 2 * direction + 1]).reshape(rows, width)
            log_a = -8.0 * rate * jax.nn.softplus(-decay_logit[layer, direction])
            decay = jnp.exp(log_a)
            drive = jnp.sqrt(-jnp.expm1(2.0 * log_a)) * inp * conv32
            prod_a, state = lax.associative_scan(
                combine_pair, (decay, drive), reverse=direction == 1, axis=0
            )
            locals_a.append(prod_a)
            locals_h.append(state)
        summary = jnp.stack([locals_a[0][-1], locals_h[0][-1], locals_a[1][0], locals_h[1][0]])[
            None
        ]
        every = lax.all_gather(summary, "sp", axis=0, tiled=True)
        count = every.shape[0]
        me = lax.axis_index("sp")
        _, incl_f = lax.associative_scan(combine_pair, (every[:, 0], every[:, 1]), axis=0)
        _, incl_b = lax.associative_scan(
            combine_pair, (every[:, 2], every[:, 3]), reverse=True, axis=0
        )
        before = lax.dynamic_index_in_dim(incl_f, jnp.maximum(me - 1, 0), 0, keepdims=False)
        after = lax.dynamic_index_in_dim(incl_b, jnp.minimum(me + 1, count - 1), 0, keepdims=False)
        carry_f = before * (me > 0).astype(jnp.float32)
        carry_b = after * (me < count - 1).astype(jnp.float32)
        hidden = locals_h[0] + locals_a[0] * carry_f + locals_h[1] + locals_a[1] * carry_b
        mix = (jax.nn.gelu(gin.astype(jnp.float32)) * hidden).astype(jnp.bfloat16)
        full_mix = lax.all_gather(mix, "tp", axis=1, tiled=True)
        out = jnp.dot(
            full_mix,
            lax.all_gather(out_weight[layer], "sp", axis=0, tiled=True),
            preferred_element_type=jnp.float32,
        )
        resid = (resid.astype(jnp.float32) + out).astype(jnp.bfloat16)
    wide = resid.astype(jnp.float32)
    total = lax.psum(jnp.sum(wide * wide, axis=1), "tp")
    scale = lax.rsqrt(total / D + EPS)
    return (wide * scale[:, None] * final_gain).astype(jnp.bfloat16)


def solution(mesh):
    placed = (
        P(("grp", "sp"), "tp"),
        P(),
        P(None, "sp", "tp"),
        P(None, "sp", "tp"),
        P(None, None, "tp"),
        P(None, None, "tp"),
        P(None, "tp", "sp"),
        P(None, "sp", "tp"),
        P("tp"),
    )
    n = mesh.shape["sp"]
    square = n == mesh.shape["tp"] and n == 4 and HEAD_W % (D // (n * n)) == 0
    return jax.shard_map(
        body_square if square else body,
        mesh=mesh,
        in_specs=placed,
        out_specs=P(("grp", "sp"), "tp"),
        check_vma=False,
    )
```
